512 devices in a mesh: grp: 2 (over y), fs: 32 (over z), tp: 8 (over x, core).
Axes of the slice: x: 4, y: 2, z: 32, core: 2. Of those that a mesh axis runs over, the one named last changes fastest.
The devices are a block of a 4x8x32 slice.
Arguments:
- tokens: bfloat16 [32768, 2048], P(('grp', 'fs'), 'tp'), parts along dimension 0, may hold values from -6 to 6
- first_gain: bfloat16 [2048], replicated, may hold values from 0.099609375 to 1.8984375
- u_proj: bfloat16 [2048, 1024], P('fs', 'tp'), may hold values from -0.125 to 0.125
- v_proj: bfloat16 [2048, 1024], P('fs', 'tp'), may hold values from -0.125 to 0.125
- group_gain: bfloat16 [8, 128], P('tp'), may hold values from 0.099609375 to 1.8984375
- spatial: bfloat16 [8, 128, 128], P('tp'), may hold values from -0.5 to 0.5
- spatial_bias: bfloat16 [8, 128], P('tp'), may hold values from 0.099609375 to 1.8984375
- mix_proj: bfloat16 [1024, 2048], P('fs', 'tp'), may hold values from -0.1875 to 0.1875
- second_gain: bfloat16 [2048], replicated, may hold values from 0.099609375 to 1.8984375
- up_proj: bfloat16 [2048, 8192], P('fs', 'tp'), may hold values from -0.125 to 0.125
- down_proj: bfloat16 [8192, 2048], P('tp', 'fs'), may hold values from -0.0625 to 0.0625
Outputs:
- layer_out: bfloat16 [32768, 2048], P(('grp', 'fs'), 'tp'), parts along dimension 0
The draws below stay inside these ranges and needn't reach their ends.
There are 2 independent parts, one for each index of `grp`. The reference program is written for one: setup_inputs(seed, part) draws one part's arguments, and reference() takes and returns one part's arrays. A program takes and returns all parts, laid end to end along the dimension named above; an argument that names none is the same for every part. Nothing has to cross between parts.
All inputs are finite; a program needn't handle non-finite values.
Results may differ from the reference program's by a relative error of at most 0.017.
Values may be sent and summed in bfloat16 or wider, within the bound.
No kernel may reach another device: no remote copies, remote signals or barrier semaphores. Data moves between devices by JAX's collectives and lax.ppermute only.
A program may use at most 64 MiB of HBM per device.

```python
import jax
import jax.numpy as jnp
from jax import lax

D = 2048
GROUPS = 8
GROUP_DIM = 128
FF = 8192
BLOCK = 128
D_A = 1024
FF_DEV = 1024
TOKENS = 16384


def level_of(key, extent, cuts, least, high):
    level, own = 1.0, jax.random.fold_in(key, 6)
    for dim, shards_of in cuts:
        steps = jnp.exp(jax.random.uniform(jax.random.fold_in(own, dim), (shards_of,), jnp.float32, least / len(cuts), high / len(cuts)))
        level = level * jnp.repeat(steps, extent[dim] // shards_of).reshape([-1 if axis == dim else 1 for axis in range(len(extent))])
    return level


def bell_draw(own_key, extent, width, limit, split=(), kind=jnp.bfloat16):
    values = jax.random.normal(own_key, extent, jnp.float32) * width
    if len(split) > 0:
        values = level_of(own_key, extent, split, -0.22, 0.18) * values
    return jnp.clip(values, min=-limit, max=limit).astype(kind)


def setup_inputs(seed: int = 0, part: int = 0) -> dict:
    arg_keys = jax.random.split(jax.random.key(seed), 12)
    part_keys = jax.random.split(jax.random.fold_in(arg_keys[11], part), 12)
    return {
        "tokens": bell_draw(part_keys[0], (TOKENS, D), 1.0, 6.0, ((0, 32), (1, 8))),
        "first_gain": jnp.clip(1.0 + 0.18 * jax.random.normal(arg_keys[1], (D,), jnp.float32), 0.099609375, 1.8984375).astype(jnp.bfloat16),
        "u_proj": bell_draw(arg_keys[2], (D, D_A), D ** -0.5, 0.125, ((0, 32), (1, 8))),
        "v_proj": bell_draw(arg_keys[3], (D, D_A), D ** -0.5, 0.125, ((0, 32), (1, 8))),
        "group_gain": jnp.clip(1.0 + 0.18 * jax.random.normal(arg_keys[4], (GROUPS, GROUP_DIM), jnp.float32), 0.099609375, 1.8984375).astype(jnp.bfloat16),
        "spatial": bell_draw(arg_keys[5], (GROUPS, BLOCK, BLOCK), BLOCK ** -0.5, 0.5, ((0, 8),)),
        "spatial_bias": jnp.clip(1.0 + 0.18 * jax.random.normal(arg_keys[6], (GROUPS, BLOCK), jnp.float32), 0.099609375, 1.8984375).astype(jnp.bfloat16),
        "mix_proj": bell_draw(arg_keys[7], (D_A, D), D_A ** -0.5, 0.1875, ((0, 32), (1, 8))),
        "second_gain": jnp.clip(1.0 + 0.18 * jax.random.normal(arg_keys[8], (D,), jnp.float32), 0.099609375, 1.8984375).astype(jnp.bfloat16),
        "up_proj": bell_draw(arg_keys[9], (D, FF), D ** -0.5, 0.125, ((0, 32), (1, 8))),
        "down_proj": bell_draw(arg_keys[10], (FF, D), FF ** -0.5, 0.0625, ((0, 8), (1, 32))),
    }


EPS = 1e-06

def rms_scale(values, gain_vec):
    mean_sq = lax.optimization_barrier(jnp.mean(values * values, axis=-1, keepdims=True))
    return values * lax.rsqrt(mean_sq + EPS) * gain_vec.astype(jnp.float32)

def reference(tokens, first_gain, u_proj, v_proj, group_gain, spatial, spatial_bias, mix_proj, second_gain, up_proj, down_proj):
    row_count = tokens.shape[0]
    residual = tokens.astype(jnp.float32)
    normed_rows = rms_scale(residual, first_gain).astype(jnp.bfloat16)
    u_act = jax.nn.gelu(jnp.dot(normed_rows, u_proj, preferred_element_type=jnp.float32)).astype(jnp.bfloat16)
    v_act = jax.nn.gelu(jnp.dot(normed_rows, v_proj, preferred_element_type=jnp.float32))
    v_groups = v_act.reshape(row_count, GROUPS, GROUP_DIM)
    v_normed = rms_scale(v_groups, group_gain).astype(jnp.bfloat16)
    block_view = v_normed.reshape(row_count // BLOCK, BLOCK, GROUPS, GROUP_DIM)
    causal_mask = jnp.tril(jnp.ones((BLOCK, BLOCK), jnp.bool_))
    masked_weights = jnp.where(causal_mask[None], spatial, jnp.zeros_like(spatial))
    mixed_vals = jnp.einsum('gts,nsgd->ntgd', masked_weights.astype(jnp.float32), block_view.astype(jnp.float32))
    mixed_vals = mixed_vals + spatial_bias.astype(jnp.float32).T[None, :, :, None]
    gated_vals = (u_act.astype(jnp.float32) * mixed_vals.reshape(row_count, GROUPS * GROUP_DIM)).astype(jnp.bfloat16)
    mix_vals = jnp.dot(gated_vals, mix_proj, preferred_element_type=jnp.float32)
    mid_stream = (residual + mix_vals).astype(jnp.bfloat16)
    normed_two = rms_scale(mid_stream.astype(jnp.float32), second_gain).astype(jnp.bfloat16)
    pre_act = jnp.dot(normed_two, up_proj, preferred_element_type=jnp.float32)
    hidden_act = jnp.square(jax.nn.relu(pre_act)).astype(jnp.bfloat16)
    down_sum = jnp.zeros((row_count, D), jnp.float32)
    for block_idx in range(FF // FF_DEV):
        first_row = block_idx * FF_DEV
        partial_prod = jnp.dot(hidden_act[:, first_row:first_row + FF_DEV], down_proj[first_row:first_row + FF_DEV], preferred_element_type=jnp.float32)
        rounded_part = lax.optimization_barrier(partial_prod.astype(jnp.bfloat16))
        down_sum = down_sum + rounded_part.astype(jnp.float32)
    return (mid_stream.astype(jnp.float32) + down_sum).astype(jnp.bfloat16)
```

```python
import jax
import jax.numpy as jnp
from jax import lax
from jax.sharding import PartitionSpec as P

EPS = 1e-06


def rms_scale(values, gain_vec):
    mean_sq = jnp.mean(values * values, axis=-1, keepdims=True)
    return values * lax.rsqrt(mean_sq + EPS) * gain_vec.astype(jnp.float32)


def sent_to_all(shard, axis):
    copies = jnp.broadcast_to(shard, (lax.axis_size(axis), *shard.shape))
    return lax.all_to_all(copies, axis, split_axis=0, concat_axis=0, tiled=True)


def in_order(blocks, dim):
    blocks = jnp.moveaxis(blocks, 0, dim)
    lengths = blocks.shape
    return blocks.reshape(*lengths[:dim], lengths[dim] * lengths[dim + 1], *lengths[dim + 2 :])


def split_up(shard, dim, size):
    lengths = shard.shape
    blocks = shard.reshape(*lengths[:dim], size, lengths[dim] // size, *lengths[dim + 1 :])
    return jnp.moveaxis(blocks, dim, 0)


def sum_at_owner(shard, axis, dim):
    size = lax.axis_size(axis)
    blocks = lax.all_to_all(split_up(shard, dim, size), axis, 0, 0, tiled=True)
    return jnp.sum(blocks.astype(jnp.float32), axis=0)


def shift(x, axis, by):
    n = lax.axis_size(axis)
    return lax.ppermute(x, axis, [(i, (i + by) % n) for i in range(n)])


def gather_two_level(shard, axis):
    n = lax.axis_size(axis)
    half = n // 2
    own = lax.all_gather(
        shard, axis, axis=0, tiled=False,
        axis_index_groups=[[r + 2 * i for i in range(half)] for r in range(2)],
    )
    cut = half // 2
    from_left = shift(own[:cut], axis, 1)
    from_right = shift(own[cut:], axis, -1)
    other = jnp.concatenate([from_left, from_right], 0)
    odd = lax.axis_index(axis) % 2 == 1
    even_set = jnp.where(odd, other, own)
    odd_set = jnp.where(odd, own, other)
    return jnp.stack([even_set, odd_set], 1).reshape(n, *shard.shape)


def swap_cores(x, axis):
    n = lax.axis_size(axis)
    return lax.ppermute(x, axis, [(i, i ^ 1) for i in range(n)])


def gather_chips(x, axis):
    n = lax.axis_size(axis)
    return lax.all_gather(
        x, axis, axis=0, tiled=False,
        axis_index_groups=[[2 * i + c for i in range(n // 2)] for c in range(2)],
    )


def pair_up(mine, theirs, axis):
    second = lax.axis_index(axis) % 2 == 1
    first_core = jnp.where(second, theirs, mine)
    second_core = jnp.where(second, mine, theirs)
    both = jnp.stack([first_core, second_core], 1)
    return both.reshape(-1, *mine.shape[1:])


def per_device(
    tokens,
    first_gain,
    u_proj,
    v_proj,
    group_gain,
    spatial,
    spatial_bias,
    mix_proj,
    second_gain,
    up_proj,
    down_proj,
):
    ffn_w = lax.all_gather(jnp.stack([up_proj, down_proj.T]), "fs", axis=1, tiled=True)
    whole_rows = in_order(sent_to_all(tokens, "tp"), 1)
    small = jnp.concatenate([jnp.concatenate([u_proj, v_proj], 1), mix_proj], 0)
    small_all = gather_two_level(small, "fs")
    rows_uv = u_proj.shape[0]
    width = u_proj.shape[1]
    uv = small_all[:, :rows_uv].reshape(-1, 2 * width)
    mix = small_all[:, rows_uv:].reshape(-1, mix_proj.shape[1])

    row_count = whole_rows.shape[0]
    normed_rows = rms_scale(whole_rows.astype(jnp.float32), first_gain).astype(jnp.bfloat16)
    uv_pre = jnp.dot(normed_rows, uv, preferred_element_type=jnp.float32)
    u_act = jax.nn.gelu(uv_pre[:, :width]).astype(jnp.bfloat16)
    local_groups, group_width = group_gain.shape
    v_groups = jax.nn.gelu(uv_pre[:, width:]).reshape(row_count, local_groups, group_width)
    v_normed = rms_scale(v_groups, group_gain).astype(jnp.bfloat16)
    block_len = spatial.shape[1]
    block_view = v_normed.reshape(row_count // block_len, block_len, local_groups, group_width)
    causal_mask = jnp.tril(jnp.ones((block_len, block_len), jnp.bool_))
    masked_weights = jnp.where(causal_mask[None], spatial, jnp.zeros_like(spatial))
    mixed_vals = jnp.einsum(
        "gts,nsgd->ntgd", masked_weights, block_view, preferred_element_type=jnp.float32
    )
    mixed_vals = mixed_vals + spatial_bias.astype(jnp.float32).T[None, :, :, None]
    gated_vals = (u_act.astype(jnp.float32) * mixed_vals.reshape(row_count, width)).astype(
        jnp.bfloat16
    )
    g_mine = gather_chips(gated_vals, "tp")
    gated_whole = in_order(pair_up(g_mine, swap_cores(g_mine, "tp"), "tp"), 1)
    mix_vals = jnp.dot(gated_whole, mix, preferred_element_type=jnp.float32)
    mid_stream = (tokens.astype(jnp.float32) + mix_vals).astype(jnp.bfloat16)
    cut = row_count // 2
    m_mine = jnp.concatenate(
        [gather_chips(mid_stream[:cut], "tp"), gather_chips(mid_stream[cut:], "tp")], 1
    )
    mid_whole = in_order(pair_up(m_mine, swap_cores(m_mine, "tp"), "tp"), 1)
    normed_two = rms_scale(mid_whole.astype(jnp.float32), second_gain).astype(jnp.bfloat16)
    pre_act = jnp.dot(normed_two, ffn_w[0], preferred_element_type=jnp.float32)
    hidden_act = jnp.square(jax.nn.relu(pre_act)).astype(jnp.bfloat16)
    down_terms = lax.dot_general(
        hidden_act, ffn_w[1], (((1,), (1,)), ((), ())), preferred_element_type=jnp.float32
    )
    down_sum = sum_at_owner(down_terms.astype(jnp.bfloat16), "tp", 1)
    return (mid_stream.astype(jnp.float32) + down_sum).astype(jnp.bfloat16)


def solution(mesh):
    return jax.shard_map(
        per_device,
        mesh=mesh,
        in_specs=(
            P(("grp", "fs"), "tp"),
            P(),
            P("fs", "tp"),
            P("fs", "tp"),
            P("tp", None),
            P("tp", None, None),
            P("tp", None),
            P("fs", "tp"),
            P(),
            P("fs", "tp"),
            P("tp", "fs"),
        ),
        out_specs=P(("grp", "fs"), "tp"),
        check_vma=False,
    )
```

```python
import jax
import jax.numpy as jnp
from jax import lax
from jax.experimental import pallas as pl
from jax.experimental.pallas import tpu as pltpu
from jax.sharding import PartitionSpec as P

EPS = 1e-06


def rms_scale(values, gain_vec):
    mean_sq = jnp.mean(values * values, axis=-1, keepdims=True)
    return values * lax.rsqrt(mean_sq + EPS) * gain_vec.astype(jnp.float32)


def sent_to_all(shard, axis):
    copies = jnp.broadcast_to(shard, (lax.axis_size(axis), *shard.shape))
    return lax.all_to_all(copies, axis, split_axis=0, concat_axis=0, tiled=True)


def in_order(blocks, dim):
    blocks = jnp.moveaxis(blocks, 0, dim)
    lengths = blocks.shape
    return blocks.reshape(*lengths[:dim], lengths[dim] * lengths[dim + 1], *lengths[dim + 2 :])


def shift(x, axis, by):
    n = lax.axis_size(axis)
    return lax.ppermute(x, axis, [(i, (i + by) % n) for i in range(n)])


def gather_two_level(shard, axis):
    n = lax.axis_size(axis)
    half = n // 2
    own = lax.all_gather(
        shard, axis, axis=0, tiled=False,
        axis_index_groups=[[r + 2 * i for i in range(half)] for r in range(2)],
    )
    cut = half // 2
    from_left = shift(own[:cut], axis, 1)
    from_right = shift(own[cut:], axis, -1)
    other = jnp.concatenate([from_left, from_right], 0)
    odd = lax.axis_index(axis) % 2 == 1
    even_set = jnp.where(odd, other, own)
    odd_set = jnp.where(odd, own, other)
    return jnp.stack([even_set, odd_set], 1).reshape(n, *shard.shape)


def swap_cores(x, axis):
    n = lax.axis_size(axis)
    return lax.ppermute(x, axis, [(i, i ^ 1) for i in range(n)])


def chip_groups(axis):
    n = lax.axis_size(axis)
    return [[2 * i + c for i in range(n // 2)] for c in range(2)]


def exchange_chips(blocks, axis):
    return lax.all_to_all(
        blocks, axis, split_axis=0, concat_axis=0, tiled=True,
        axis_index_groups=chip_groups(axis),
    )


NT = (((1,), (1,)), ((), ()))


def mix_kernel(core_ref, mine_ref, theirs_ref, mix_ref, tok_ref, out_ref):
    core = core_ref[0]
    chips = mine_ref.shape[0]
    total = tok_ref[...].astype(jnp.float32)
    for x in range(chips):
        total += jnp.dot(mine_ref[x], mix_ref[2 * x + core], preferred_element_type=jnp.float32)
        total += jnp.dot(
            theirs_ref[x], mix_ref[2 * x + 1 - core], preferred_element_type=jnp.float32
        )
    mid = total.astype(out_ref.dtype)
    for x in range(chips):
        out_ref[x] = mid


def mix_to_mid(core, mine, theirs, mix, tokens):
    chips, rows, width = mine.shape
    cols = tokens.shape[1]
    step = rows // 4
    return pl.pallas_call(
        mix_kernel,
        grid_spec=pltpu.PrefetchScalarGridSpec(
            num_scalar_prefetch=1,
            grid=(4,),
            in_specs=[
                pl.BlockSpec((chips, step, width), lambda i, c: (0, i, 0)),
                pl.BlockSpec((chips, step, width), lambda i, c: (0, i, 0)),
                pl.BlockSpec((2 * chips, width, cols), lambda i, c: (0, 0, 0)),
                pl.BlockSpec((step, cols), lambda i, c: (i, 0)),
            ],
            out_specs=pl.BlockSpec((chips, step, cols), lambda i, c: (0, i, 0)),
        ),
        out_shape=jax.ShapeDtypeStruct((chips, rows, cols), tokens.dtype),
        cost_estimate=pl.CostEstimate(
            flops=4 * chips * rows * width * cols, bytes_accessed=4 << 20, transcendentals=0
        ),
    )(core, mine, theirs, mix.reshape(2 * chips, width, cols), tokens)


def norm_kernel(core_ref, mine_ref, theirs_ref, gain_ref, out_ref):
    core = core_ref[0]
    chips, _, cols = mine_ref.shape
    square = 0.0
    for x in range(chips):
        a = mine_ref[x].astype(jnp.float32)
        b = theirs_ref[x].astype(jnp.float32)
        square += jnp.sum(a * a + b * b, axis=1, keepdims=True)
    scale = lax.rsqrt(square / (2 * chips * cols) + EPS)
    for x in range(chips):
        for ref, c in ((mine_ref, core), (theirs_ref, 1 - core)):
            at = pl.ds(pl.multiple_of((2 * x + c) * cols, cols), cols)
            gain = gain_ref[:, at].astype(jnp.float32)
            out_ref[:, at] = (ref[x].astype(jnp.float32) * scale * gain).astype(out_ref.dtype)


def norm_pieces(core, mine, theirs, gain):
    chips, rows, cols = mine.shape
    step = rows // 4
    whole = 2 * chips * cols
    return pl.pallas_call(
        norm_kernel,
        grid_spec=pltpu.PrefetchScalarGridSpec(
            num_scalar_prefetch=1,
            grid=(4,),
            in_specs=[
                pl.BlockSpec((chips, step, cols), lambda i, c: (0, i, 0)),
                pl.BlockSpec((chips, step, cols), lambda i, c: (0, i, 0)),
                pl.BlockSpec((1, whole), lambda i, c: (0, 0)),
            ],
            out_specs=pl.BlockSpec((step, whole), lambda i, c: (i, 0)),
        ),
        out_shape=jax.ShapeDtypeStruct((rows, whole), mine.dtype),
        cost_estimate=pl.CostEstimate(
            flops=8 * rows * whole, bytes_accessed=4 * rows * whole, transcendentals=rows
        ),
    )(core, mine, theirs, gain.reshape(1, whole))


def ffn_kernel(core_ref, x_ref, up_ref, down_ref, own_ref, theirs_ref, hid_ref):
    i = pl.program_id(0)
    chunk = up_ref.shape[2]
    ups = hid_ref.shape[1] // chunk

    @pl.when(i < ups)
    def _():
        pre = jnp.dot(x_ref[...], up_ref[0], preferred_element_type=jnp.float32)
        act = jnp.square(jnp.maximum(pre, 0.0)).astype(hid_ref.dtype)
        hid_ref[:, pl.ds(pl.multiple_of(i * chunk, chunk), chunk)] = act

    @pl.when(i >= ups)
    def _():
        both = lax.dot_general(
            hid_ref[...], down_ref[0, 0], NT, preferred_element_type=jnp.float32
        ).astype(own_ref.dtype)
        cols = own_ref.shape[2]
        first, second = both[:, :cols], both[:, cols:]

        @pl.when(core_ref[0] == 0)
        def _():
            own_ref[0] = first
            theirs_ref[0] = second

        @pl.when(core_ref[0] == 1)
        def _():
            own_ref[0] = second
            theirs_ref[0] = first


def ffn_partials(core, x, weights, chips):
    rows, width = x.shape
    units = weights.shape[2]
    cols = width // (2 * chips)
    chunk = units // 4
    ups = units // chunk
    pieces = weights.reshape(2, chips, 2 * cols, units)

    out_spec = pl.BlockSpec((1, rows, cols), lambda i, p: (jnp.maximum(i - ups, 0), 0, 0))
    return pl.pallas_call(
        ffn_kernel,
        grid_spec=pltpu.PrefetchScalarGridSpec(
            num_scalar_prefetch=1,
            grid=(ups + chips,),
            in_specs=[
                pl.BlockSpec((rows, width), lambda i, p: (0, 0)),
                pl.BlockSpec((1, width, chunk), lambda i, p: (0, 0, jnp.minimum(i, ups - 1))),
                pl.BlockSpec((1, 1, 2 * cols, units), lambda i, p: (1, jnp.maximum(i - ups, 0), 0, 0)),
            ],
            out_specs=[out_spec, out_spec],
            scratch_shapes=[pltpu.VMEM((rows, units), x.dtype)],
        ),
        out_shape=[jax.ShapeDtypeStruct((chips, rows, cols), x.dtype)] * 2,
        cost_estimate=pl.CostEstimate(
            flops=4 * rows * width * units, bytes_accessed=12 << 20, transcendentals=0
        ),
    )(core, x, weights, pieces)


def sum_at_owners(own, theirs, axis):
    received = swap_cores(theirs, axis)
    pair_sum = (own.astype(jnp.float32) + received.astype(jnp.float32)).astype(own.dtype)
    parts = exchange_chips(pair_sum, axis)
    return jnp.sum(parts.astype(jnp.float32), axis=0)


def per_device(
    tokens,
    first_gain,
    u_proj,
    v_proj,
    group_gain,
    spatial,
    spatial_bias,
    mix_proj,
    second_gain,
    up_proj,
    down_proj,
):
    ffn_w = lax.all_gather(jnp.stack([up_proj, down_proj.T]), "fs", axis=1, tiled=True)
    whole_rows = in_order(sent_to_all(tokens, "tp"), 1)
    small = jnp.concatenate([jnp.concatenate([u_proj, v_proj], 1), mix_proj], 0)
    small_all = gather_two_level(small, "fs")
    rows_uv = u_proj.shape[0]
    width = u_proj.shape[1]
    uv = small_all[:, :rows_uv].reshape(-1, 2 * width)
    mix = small_all[:, rows_uv:].reshape(-1, mix_proj.shape[1])

    row_count = whole_rows.shape[0]
    normed_rows = rms_scale(whole_rows.astype(jnp.float32), first_gain).astype(jnp.bfloat16)
    uv_pre = jnp.dot(normed_rows, uv, preferred_element_type=jnp.float32)
    u_act = jax.nn.gelu(uv_pre[:, :width]).astype(jnp.bfloat16)
    local_groups, group_width = group_gain.shape
    v_groups = jax.nn.gelu(uv_pre[:, width:]).reshape(row_count, local_groups, group_width)
    v_normed = rms_scale(v_groups, group_gain).astype(jnp.bfloat16)
    block_len = spatial.shape[1]
    block_view = v_normed.reshape(row_count // block_len, block_len, local_groups, group_width)
    causal_mask = jnp.tril(jnp.ones((block_len, block_len), jnp.bool_))
    masked_weights = jnp.where(causal_mask[None], spatial, jnp.zeros_like(spatial))
    mixed_vals = jnp.einsum(
        "gts,nsgd->ntgd", masked_weights, block_view, preferred_element_type=jnp.float32
    )
    mixed_vals = mixed_vals + spatial_bias.astype(jnp.float32).T[None, :, :, None]
    gated_vals = (u_act.astype(jnp.float32) * mixed_vals.reshape(row_count, width)).astype(
        jnp.bfloat16
    )
    chips = lax.axis_size("tp") // 2
    core = jnp.reshape(lax.axis_index("tp") % 2, (1,)).astype(jnp.int32)
    g_mine = exchange_chips(jnp.broadcast_to(gated_vals, (chips, *gated_vals.shape)), "tp")
    g_theirs = swap_cores(g_mine, "tp")
    mid_copies = mix_to_mid(core, g_mine, g_theirs, mix, tokens)
    m_mine = exchange_chips(mid_copies, "tp")
    m_theirs = swap_cores(m_mine, "tp")
    normed_two = norm_pieces(core, m_mine, m_theirs, second_gain)
    own, theirs = ffn_partials(core, normed_two, ffn_w, chips)
    down_sum = sum_at_owners(own, theirs, "tp")
    return (mid_copies[0].astype(jnp.float32) + down_sum).astype(jnp.bfloat16)


def solution(mesh):
    return jax.shard_map(
        per_device,
        mesh=mesh,
        in_specs=(
            P(("grp", "fs"), "tp"),
            P(),
            P("fs", "tp"),
            P("fs", "tp"),
            P("tp", None),
            P("tp", None, None),
            P("tp", None),
            P("fs", "tp"),
            P(),
            P("fs", "tp"),
            P("tp", "fs"),
        ),
        out_specs=P(("grp", "fs"), "tp"),
        check_vma=False,
    )
```

```python
import jax
import jax.numpy as jnp
from jax import lax
from jax.experimental import pallas as pl
from jax.experimental.pallas import tpu as pltpu
from jax.sharding import PartitionSpec as P

EPS = 1e-06


def rms_scale(values, gain_vec):
    mean_sq = jnp.mean(values * values, axis=-1, keepdims=True)
    return values * lax.rsqrt(mean_sq + EPS) * gain_vec.astype(jnp.float32)


def sent_to_all(shard, axis):
    copies = jnp.broadcast_to(shard, (lax.axis_size(axis), *shard.shape))
    return lax.all_to_all(copies, axis, split_axis=0, concat_axis=0, tiled=True)


def in_order(blocks, dim):
    blocks = jnp.moveaxis(blocks, 0, dim)
    lengths = blocks.shape
    return blocks.reshape(*lengths[:dim], lengths[dim] * lengths[dim + 1], *lengths[dim + 2 :])


def shift(x, axis, by):
    n = lax.axis_size(axis)
    return lax.ppermute(x, axis, [(i, (i + by) % n) for i in range(n)])


def own_parity(shard, axis):
    n = lax.axis_size(axis)
    return lax.all_gather(
        shard, axis, axis=0, tiled=False,
        axis_index_groups=[[r + 2 * i for i in range(n // 2)] for r in range(2)],
    )


def gather_two_level(shard, axis, twin_axis):
    n = lax.axis_size(axis)
    half = n // 2
    twins = lax.axis_size(twin_axis)
    if twins % 2 == 0:
        rows = shard.shape[0] // 2
        upper = lax.axis_index(twin_axis) % 2 == 1
        mine = own_parity(jnp.where(upper, shard[rows:], shard[:rows]), axis)
        theirs = lax.ppermute(mine, twin_axis, [(i, i ^ 1) for i in range(twins)])
        own = jnp.concatenate(
            [jnp.where(upper, theirs, mine), jnp.where(upper, mine, theirs)], 1
        )
    else:
        own = own_parity(shard, axis)
    cut = half // 2
    from_left = shift(own[:cut], axis, 1)
    from_right = shift(own[cut:], axis, -1)
    other = jnp.concatenate([from_left, from_right], 0)
    odd = lax.axis_index(axis) % 2 == 1
    even_set = jnp.where(odd, other, own)
    odd_set = jnp.where(odd, own, other)
    return jnp.stack([even_set, odd_set], 1).reshape(n, *shard.shape)


def swap_cores(x, axis):
    n = lax.axis_size(axis)
    return lax.ppermute(x, axis, [(i, i ^ 1) for i in range(n)])


def chip_groups(axis):
    n = lax.axis_size(axis)
    return [[2 * i + c for i in range(n // 2)] for c in range(2)]


def exchange_chips(blocks, axis):
    return lax.all_to_all(
        blocks, axis, split_axis=0, concat_axis=0, tiled=True,
        axis_index_groups=chip_groups(axis),
    )


NT = (((1,), (1,)), ((), ()))


def mix_kernel(core_ref, mine_ref, theirs_ref, mix_ref, tok_ref, out_ref):
    core = core_ref[0]
    chips = mine_ref.shape[0]
    total = tok_ref[...].astype(jnp.float32)
    for x in range(chips):
        total += jnp.dot(mine_ref[x], mix_ref[2 * x + core], preferred_element_type=jnp.float32)
        total += jnp.dot(
            theirs_ref[x], mix_ref[2 * x + 1 - core], preferred_element_type=jnp.float32
        )
    mid = total.astype(out_ref.dtype)
    for x in range(chips):
        out_ref[x] = mid


def mix_to_mid(core, mine, theirs, mix, tokens):
    chips, rows, width = mine.shape
    cols = tokens.shape[1]
    step = rows // 4
    return pl.pallas_call(
        mix_kernel,
        grid_spec=pltpu.PrefetchScalarGridSpec(
            num_scalar_prefetch=1,
            grid=(4,),
            in_specs=[
                pl.BlockSpec((chips, step, width), lambda i, c: (0, i, 0)),
                pl.BlockSpec((chips, step, width), lambda i, c: (0, i, 0)),
                pl.BlockSpec((2 * chips, width, cols), lambda i, c: (0, 0, 0)),
                pl.BlockSpec((step, cols), lambda i, c: (i, 0)),
            ],
            out_specs=pl.BlockSpec((chips, step, cols), lambda i, c: (0, i, 0)),
        ),
        out_shape=jax.ShapeDtypeStruct((chips, rows, cols), tokens.dtype),
        cost_estimate=pl.CostEstimate(
            flops=4 * chips * rows * width * cols, bytes_accessed=4 << 20, transcendentals=0
        ),
    )(core, mine, theirs, mix.reshape(2 * chips, width, cols), tokens)


def norm_kernel(core_ref, mine_ref, theirs_ref, gain_ref, out_ref):
    core = core_ref[0]
    chips, _, cols = mine_ref.shape
    square = 0.0
    for x in range(chips):
        a = mine_ref[x].astype(jnp.float32)
        b = theirs_ref[x].astype(jnp.float32)
        square += jnp.sum(a * a + b * b, axis=1, keepdims=True)
    scale = lax.rsqrt(square / (2 * chips * cols) + EPS)
    for x in range(chips):
        for ref, c in ((mine_ref, core), (theirs_ref, 1 - core)):
            at = pl.ds(pl.multiple_of((2 * x + c) * cols, cols), cols)
            gain = gain_ref[:, at].astype(jnp.float32)
            out_ref[:, at] = (ref[x].astype(jnp.float32) * scale * gain).astype(out_ref.dtype)


def norm_pieces(core, mine, theirs, gain):
    chips, rows, cols = mine.shape
    step = rows // 4
    whole = 2 * chips * cols
    return pl.pallas_call(
        norm_kernel,
        grid_spec=pltpu.PrefetchScalarGridSpec(
            num_scalar_prefetch=1,
            grid=(4,),
            in_specs=[
                pl.BlockSpec((chips, step, cols), lambda i, c: (0, i, 0)),
                pl.BlockSpec((chips, step, cols), lambda i, c: (0, i, 0)),
                pl.BlockSpec((1, whole), lambda i, c: (0, 0)),
            ],
            out_specs=pl.BlockSpec((step, whole), lambda i, c: (i, 0)),
        ),
        out_shape=jax.ShapeDtypeStruct((rows, whole), mine.dtype),
        cost_estimate=pl.CostEstimate(
            flops=8 * rows * whole, bytes_accessed=4 * rows * whole, transcendentals=rows
        ),
    )(core, mine, theirs, gain.reshape(1, whole))


def ffn_kernel(core_ref, x_ref, up_ref, down_ref, own_ref, theirs_ref, hid_ref):
    i = pl.program_id(0)
    chunk = up_ref.shape[2]
    ups = hid_ref.shape[1] // chunk

    @pl.when(i < ups)
    def _():
        pre = jnp.dot(x_ref[...], up_ref[0], preferred_element_type=jnp.float32)
        act = jnp.square(jnp.maximum(pre, 0.0)).astype(hid_ref.dtype)
        hid_ref[:, pl.ds(pl.multiple_of(i * chunk, chunk), chunk)] = act

    @pl.when(i >= ups)
    def _():
        both = lax.dot_general(
            hid_ref[...], down_ref[0, 0], NT, preferred_element_type=jnp.float32
        ).astype(own_ref.dtype)
        cols = own_ref.shape[2]
        first, second = both[:, :cols], both[:, cols:]

        @pl.when(core_ref[0] == 0)
        def _():
            own_ref[0] = first
            theirs_ref[0] = second

        @pl.when(core_ref[0] == 1)
        def _():
            own_ref[0] = second
            theirs_ref[0] = first


def ffn_partials(core, x, weights, chips):
    rows, width = x.shape
    units = weights.shape[2]
    cols = width // (2 * chips)
    chunk = units // 4
    ups = units // chunk
    pieces = weights.reshape(2, chips, 2 * cols, units)

    out_spec = pl.BlockSpec((1, rows, cols), lambda i, p: (jnp.maximum(i - ups, 0), 0, 0))
    return pl.pallas_call(
        ffn_kernel,
        grid_spec=pltpu.PrefetchScalarGridSpec(
            num_scalar_prefetch=1,
            grid=(ups + chips,),
            in_specs=[
                pl.BlockSpec((rows, width), lambda i, p: (0, 0)),
                pl.BlockSpec((1, width, chunk), lambda i, p: (0, 0, jnp.minimum(i, ups - 1))),
                pl.BlockSpec((1, 1, 2 * cols, units), lambda i, p: (1, jnp.maximum(i - ups, 0), 0, 0)),
            ],
            out_specs=[out_spec, out_spec],
            scratch_shapes=[pltpu.VMEM((rows, units), x.dtype)],
        ),
        out_shape=[jax.ShapeDtypeStruct((chips, rows, cols), x.dtype)] * 2,
        cost_estimate=pl.CostEstimate(
            flops=4 * rows * width * units, bytes_accessed=12 << 20, transcendentals=0
        ),
    )(core, x, weights, pieces)


def sum_at_owners(own, theirs, axis):
    received = swap_cores(theirs, axis)
    pair_sum = (own.astype(jnp.float32) + received.astype(jnp.float32)).astype(own.dtype)
    parts = exchange_chips(pair_sum, axis)
    return jnp.sum(parts.astype(jnp.float32), axis=0)


def per_device(
    tokens,
    first_gain,
    u_proj,
    v_proj,
    group_gain,
    spatial,
    spatial_bias,
    mix_proj,
    second_gain,
    up_proj,
    down_proj,
):
    ffn_w = lax.all_gather(jnp.stack([up_proj, down_proj.T]), "fs", axis=1, tiled=True)
    whole_rows = in_order(sent_to_all(tokens, "tp"), 1)
    small = jnp.concatenate([jnp.concatenate([u_proj, v_proj], 1), mix_proj], 0)
    small_all = gather_two_level(small, "fs", "grp")
    rows_uv = u_proj.shape[0]
    width = u_proj.shape[1]
    uv = small_all[:, :rows_uv].reshape(-1, 2 * width)
    mix = small_all[:, rows_uv:].reshape(-1, mix_proj.shape[1])

    row_count = whole_rows.shape[0]
    normed_rows = rms_scale(whole_rows.astype(jnp.float32), first_gain).astype(jnp.bfloat16)
    uv_pre = jnp.dot(normed_rows, uv, preferred_element_type=jnp.float32)
    u_act = jax.nn.gelu(uv_pre[:, :width]).astype(jnp.bfloat16)
    local_groups, group_width = group_gain.shape
    v_groups = jax.nn.gelu(uv_pre[:, width:]).reshape(row_count, local_groups, group_width)
    v_normed = rms_scale(v_groups, group_gain).astype(jnp.bfloat16)
    block_len = spatial.shape[1]
    block_view = v_normed.reshape(row_count // block_len, block_len, local_groups, group_width)
    causal_mask = jnp.tril(jnp.ones((block_len, block_len), jnp.bool_))
    masked_weights = jnp.where(causal_mask[None], spatial, jnp.zeros_like(spatial))
    mixed_vals = jnp.einsum(
        "gts,nsgd->ntgd", masked_weights, block_view, preferred_element_type=jnp.float32
    )
    mixed_vals = mixed_vals + spatial_bias.astype(jnp.float32).T[None, :, :, None]
    gated_vals = (u_act.astype(jnp.float32) * mixed_vals.reshape(row_count, width)).astype(
        jnp.bfloat16
    )
    chips = lax.axis_size("tp") // 2
    core = jnp.reshape(lax.axis_index("tp") % 2, (1,)).astype(jnp.int32)
    g_mine = exchange_chips(jnp.broadcast_to(gated_vals, (chips, *gated_vals.shape)), "tp")
    g_theirs = swap_cores(g_mine, "tp")
    mid_copies = mix_to_mid(core, g_mine, g_theirs, mix, tokens)
    m_mine = exchange_chips(mid_copies, "tp")
    m_theirs = swap_cores(m_mine, "tp")
    normed_two = norm_pieces(core, m_mine, m_theirs, second_gain)
    own, theirs = ffn_partials(core, normed_two, ffn_w, chips)
    down_sum = sum_at_owners(own, theirs, "tp")
    return (mid_copies[0].astype(jnp.float32) + down_sum).astype(jnp.bfloat16)


def solution(mesh):
    return jax.shard_map(
        per_device,
        mesh=mesh,
        in_specs=(
            P(("grp", "fs"), "tp"),
            P(),
            P("fs", "tp"),
            P("fs", "tp"),
            P("tp", None),
            P("tp", None, None),
            P("tp", None),
            P("fs", "tp"),
            P(),
            P("fs", "tp"),
            P("tp", "fs"),
        ),
        out_specs=P(("grp", "fs"), "tp"),
        check_vma=False,
    )
```
